32 devices in a mesh: sp: 4 (over z), fs: 4 (over y, x), tp: 2 (over core).
Axes of the slice: x: 2, y: 2, z: 4, core: 2. Of those that a mesh axis runs over, the one named last changes fastest.
Arguments:
- inputs: bfloat16 [4, 512, 2048], P('fs', 'sp'), may hold values from -9 to 9
- norm_gain: float32 [2048], replicated, may hold values from 0.1 to 1.9
- hg_query_w: bfloat16 [2048, 1024], P(('sp', 'fs'), 'tp'), may hold values from -0.125 to 0.125
- hg_fwd_w: bfloat16 [2048, 1024], P(('sp', 'fs'), 'tp'), may hold values from -0.125 to 0.125
- hg_bwd_w: bfloat16 [2048, 1024], P(('sp', 'fs'), 'tp'), may hold values from -0.125 to 0.125
- hg_value_w: bfloat16 [2048, 1024], P(('sp', 'fs'), 'tp'), may hold values from -0.125 to 0.125
- floor_gap: float32 [2, 1024], P(None, 'tp'), may hold values from 0 to 0.1
- hg_norm_gain: float32 [64], replicated, may hold values from 0.1 to 1.9
- df_query_w: bfloat16 [2048, 512], P(('sp', 'fs'), 'tp'), may hold values from -0.176776695 to 0.176776695
- df_key_w: bfloat16 [2048, 512], P(('sp', 'fs'), 'tp'), may hold values from -4.4194174 to 4.4194174
- df_value_w: bfloat16 [2048, 512], P(('sp', 'fs'), 'tp'), may hold values from -0.125 to 0.125
- diff_lambda: float32 [8], P('tp'), may hold values from 0.3 to 0.8
- df_norm_gain: float32 [64], replicated, may hold values from 0.1 to 1.9
- out_hg_w: bfloat16 [1024, 2048], P('tp'), may hold values from -0.15625 to 0.15625
- out_df_w: bfloat16 [512, 2048], P('tp'), may hold values from -0.15625 to 0.15625
- post_gain: float32 [2048], replicated, may hold values from 0.1 to 1.9
Outputs:
- mixed: bfloat16 [4, 512, 2048], P('fs', ('sp', 'tp'))
The draws below stay inside these ranges and needn't reach their ends.
All inputs are finite; a program needn't handle non-finite values.
Results may differ from the reference program's by a relative error of at most 0.017.
Values may be sent and summed in bfloat16 or wider, within the bound.
A program may use at most 64 MiB of HBM per device.

```python
import math
import jax
import jax.numpy as jnp
from jax import lax

D = 2048
HG_HEADS = 16
HEAD = 64
DF_HEADS = 8
DQK = 32
BLOCK = 64
TOK_DEV = 128
DFV = 64
HG_WIDTH = 1024
DF_QK_WIDTH = 512
DF_WIDTH = 512
SEQ = 512
BATCH = 4
N_TP = 2


def draw_inputs(key, part):
    base_key, shift_key = jax.random.split(key)
    base_draw = jax.random.normal(base_key, (BATCH, SEQ, D), jnp.float32)
    shifts = jax.random.normal(shift_key, (BATCH, SEQ // TOK_DEV, D), jnp.float32)
    summed = base_draw + jnp.repeat(shifts, TOK_DEV, axis=1)
    return jnp.clip(summed, -9.0, 9.0).astype(jnp.bfloat16)


def draw_floor_gap(key, part):
    kind_key, slow_key, fast_key = jax.random.split(key, 3)
    chooser = jax.random.randint(kind_key, (2, HG_HEADS, 1), 0, 10)
    is_fast = chooser < 5
    slow_gap = jnp.exp(jax.random.uniform(slow_key, (2, HG_HEADS, HEAD), jnp.float32, math.log(0.1), 0.0)) / SEQ
    fast_gap = jnp.exp(jax.random.uniform(fast_key, (2, HG_HEADS, HEAD), jnp.float32, math.log(0.03), math.log(0.1)))
    return jnp.where(is_fast, fast_gap, slow_gap).reshape(2, HG_HEADS * HEAD).astype(jnp.float32)


def query_key_pair(key):
    base_key = jax.random.fold_in(key, 17)
    first_key, second_key = jax.random.split(base_key)
    scale_w = 1.3 * D ** (-0.5)
    queries_w = jnp.clip(jax.random.normal(first_key, (D, DF_QK_WIDTH), jnp.float32), -6.0, 6.0) * scale_w
    noise_w = jnp.clip(jax.random.normal(second_key, (D, DF_QK_WIDTH), jnp.float32), -6.0, 6.0) * scale_w
    keys_w = noise_w
    return (queries_w, keys_w)


def draw_df_query_w(key, part):
    return query_key_pair(key)[0].astype(jnp.bfloat16)


def draw_df_key_w(key, part):
    return query_key_pair(key)[1].astype(jnp.bfloat16)


def levels(key, extent, shards, smallest, high):
    level, own = 1.0, jax.random.fold_in(key, 6)
    for position, parts in shards:
        heights = jnp.exp(jax.random.uniform(jax.random.fold_in(own, position), (parts,), jnp.float32, smallest / len(shards), high / len(shards)))
        level = level * jnp.repeat(heights, extent[position] // parts).reshape([-1 if axis == position else 1 for axis in range(len(extent))])
    return level


def scatter_about(key, extent, width, limit, cuts=(), kind=jnp.bfloat16):
    values = jax.random.normal(key, extent, jnp.float32) * width
    if len(cuts) > 0:
        values = levels(key, extent, cuts, -0.22, 0.18) * values
    return jnp.clip(values, min=-limit, max=limit).astype(kind)


def setup_inputs(seed: int = 0) -> dict:
    arg_keys = jax.random.split(jax.random.key(seed), 17)
    return {
        "inputs": draw_inputs(jax.random.fold_in(arg_keys[16], 71), 0),
        "norm_gain": jnp.clip(1.0 + 0.18 * jax.random.normal(arg_keys[1], (D,), jnp.float32), 0.1, 1.9),
        "hg_query_w": scatter_about(arg_keys[2], (D, HG_WIDTH), D ** -0.5, 0.125, ((0, 16), (1, 2))),
        "hg_fwd_w": scatter_about(arg_keys[3], (D, HG_WIDTH), D ** -0.5, 0.125, ((0, 16), (1, 2))),
        "hg_bwd_w": scatter_about(arg_keys[4], (D, HG_WIDTH), D ** -0.5, 0.125, ((0, 16), (1, 2))),
        "hg_value_w": scatter_about(arg_keys[5], (D, HG_WIDTH), D ** -0.5, 0.125, ((0, 16), (1, 2))),
        "floor_gap": draw_floor_gap(jax.random.fold_in(arg_keys[16], 71), 0),
        "hg_norm_gain": jnp.clip(1.0 + 0.18 * jax.random.normal(arg_keys[7], (HEAD,), jnp.float32), 0.1, 1.9),
        "df_query_w": draw_df_query_w(jax.random.fold_in(arg_keys[16], 71), 0),
        "df_key_w": draw_df_key_w(jax.random.fold_in(arg_keys[16], 71), 0),
        "df_value_w": scatter_about(arg_keys[10], (D, DF_WIDTH), D ** -0.5, 0.125, ((0, 16), (1, 2))),
        "diff_lambda": jnp.clip(0.3 + 0.5 * jax.random.uniform(arg_keys[11], (DF_HEADS,), jnp.float32) ** levels(arg_keys[11], (DF_HEADS,), ((0, 2),), -0.2, 0.2), 0.3, 0.8),
        "df_norm_gain": jnp.clip(1.0 + 0.18 * jax.random.normal(arg_keys[12], (DFV,), jnp.float32), 0.1, 1.9),
        "out_hg_w": scatter_about(arg_keys[13], (HG_WIDTH, D), (HG_WIDTH + DF_WIDTH) ** -0.5, 0.15625, ((0, 2),)),
        "out_df_w": scatter_about(arg_keys[14], (DF_WIDTH, D), (HG_WIDTH + DF_WIDTH) ** -0.5, 0.15625, ((0, 2),)),
        "post_gain": jnp.clip(1.0 + 0.18 * jax.random.normal(arg_keys[15], (D,), jnp.float32), 0.1, 1.9),
    }


epsilon = 1e-06
df_factor = 0.8

def rms_scale(values):
    return lax.rsqrt(lax.optimization_barrier(jnp.mean(values * values, axis=-1, keepdims=True)) + epsilon)

def span_scan(queries, taken, values, kept_log):
    head_count, length, key_dim = queries.shape
    blocks = length // BLOCK

    def to_blocks(tensor):
        return tensor.reshape(head_count, blocks, BLOCK, tensor.shape[-1]).transpose(1, 0, 2, 3)
    lower_mask = jnp.tril(jnp.ones((BLOCK, BLOCK), dtype=bool))[:, :, None]
    highest_precision = lax.Precision.HIGHEST

    def advance(state_stack, pieces):
        query_block, key_block, value_block, g_blk = pieces
        cumulative_log = jnp.cumsum(g_blk, axis=1)
        across_blocks = jnp.einsum('bqy,byo->bqo', query_block * jnp.exp(cumulative_log), state_stack, precision=highest_precision)
        spread = cumulative_log[:, :, None, :] - cumulative_log[:, None, :, :]
        decays = jnp.where(lower_mask, jnp.exp(jnp.where(lower_mask, spread, 0.0)), 0.0)
        scores = jnp.einsum('hik,hijk->hij', query_block, decays * key_block[:, None, :, :], precision=highest_precision)
        inside = jnp.einsum('hij,hjv->hiv', scores, value_block, precision=highest_precision)
        final_log_decay = cumulative_log[:, -1:, :]
        carried = jnp.exp(final_log_decay[:, 0, :])[..., None] * state_stack
        fresh_portion = jnp.einsum('moc,moa->mca', key_block * jnp.exp(final_log_decay - cumulative_log), value_block, precision=highest_precision)
        return (carried + fresh_portion, across_blocks + inside)
    start_state = jnp.zeros((head_count, key_dim, values.shape[-1]), jnp.float32)
    final_state, outputs = lax.scan(advance, start_state, (to_blocks(queries), to_blocks(taken), to_blocks(values), to_blocks(kept_log)))
    return (outputs.transpose(1, 0, 2, 3).reshape(head_count, length, values.shape[-1]), final_state)

def reference(inputs, norm_gain, hg_query_w, hg_fwd_w, hg_bwd_w, hg_value_w, floor_gap, hg_norm_gain, df_query_w, df_key_w, df_value_w, diff_lambda, df_norm_gain, out_hg_w, out_df_w, post_gain):

    def one_sequence(tok_rows):
        rows_float = tok_rows.astype(jnp.float32)
        normed = (rows_float * rms_scale(rows_float) * norm_gain).astype(jnp.bfloat16)

        def project(weight):
            return jnp.dot(normed, weight, preferred_element_type=jnp.float32).astype(jnp.bfloat16)

        def split_heads(tensor):
            return tensor.astype(jnp.float32).reshape(SEQ, HG_HEADS, HEAD).transpose(1, 0, 2)
        queries = jax.nn.silu(split_heads(project(hg_query_w)))
        values = split_heads(project(hg_value_w))

        def direction(weight, gap_row, flipped):
            taken = gap_row.reshape(HG_HEADS, 1, HEAD) * jax.nn.sigmoid(-split_heads(project(weight)))
            series = (queries, taken, values, jnp.log1p(-taken))
            if flipped:
                series = tuple((jnp.flip(tensor, axis=1) for tensor in series))
            outputs, final_state = span_scan(*series)
            return jnp.flip(outputs, axis=1) if flipped else outputs
        recurrent = direction(hg_fwd_w, floor_gap[0], False) + direction(hg_bwd_w, floor_gap[1], True)
        hg_out = (recurrent * rms_scale(recurrent) * hg_norm_gain).transpose(1, 0, 2).reshape(SEQ, HG_WIDTH).astype(jnp.bfloat16)
        df_queries = project(df_query_w).reshape(SEQ // BLOCK, BLOCK, DF_HEADS, 2, DQK)
        df_keys = project(df_key_w).reshape(SEQ, DF_HEADS, 2, DQK).astype(jnp.float32)
        df_values = project(df_value_w).reshape(SEQ, DF_HEADS, DFV).astype(jnp.float32)

        def attend(query_block):
            scores = jnp.einsum('qhmd,khmd->hmqk', query_block.astype(jnp.float32), df_keys) * DQK ** (-0.5)
            shifted = jnp.exp(scores - lax.optimization_barrier(jnp.max(scores, axis=-1, keepdims=True)))
            totals = lax.optimization_barrier(jnp.sum(shifted, axis=-1))
            shifted_low = lax.optimization_barrier(shifted.astype(jnp.bfloat16)).astype(jnp.float32)
            accum = jnp.einsum('hmqk,khd->hmqd', shifted_low, df_values)
            return accum / totals[..., None]
        maps = lax.map(attend, df_queries)
        weighted = maps[:, :, 0] - diff_lambda[None, :, None, None] * maps[:, :, 1]
        df_out = (weighted * rms_scale(weighted) * df_norm_gain * df_factor).transpose(0, 2, 1, 3).reshape(SEQ, DF_WIDTH).astype(jnp.bfloat16)
        hg_parts = hg_out.reshape(SEQ, N_TP, HG_WIDTH // N_TP)
        df_parts = df_out.reshape(SEQ, N_TP, DF_WIDTH // N_TP)
        hg_rows = out_hg_w.reshape(N_TP, HG_WIDTH // N_TP, D)
        df_rows = out_df_w.reshape(N_TP, DF_WIDTH // N_TP, D)
        mixture = jnp.zeros((SEQ, D), jnp.float32)
        for member in range(N_TP):
            partial_sum = jnp.dot(hg_parts[:, member], hg_rows[member], preferred_element_type=jnp.float32) + jnp.dot(df_parts[:, member], df_rows[member], preferred_element_type=jnp.float32)
            mixture = mixture + lax.optimization_barrier(partial_sum.astype(jnp.bfloat16)).astype(jnp.float32)
        return (mixture * rms_scale(mixture) * post_gain).astype(jnp.bfloat16)
    return lax.map(one_sequence, inputs)
```

```python
import functools
import math

import jax
import jax.numpy as jnp
from jax import lax
from jax.experimental import pallas as pl
from jax.experimental.pallas import tpu as pltpu
from jax.sharding import PartitionSpec as P

HEAD = 64
DQK = 32
BLOCK = 64
DFV = 64


epsilon = 1e-06
df_factor = 0.8
highest_precision = lax.Precision.HIGHEST


def rms_scale(values):
    return lax.rsqrt(jnp.mean(values * values, axis=-1, keepdims=True) + epsilon)


def span_scan(queries, taken, values, kept_log):
    head_count, length, key_dim = queries.shape
    blocks = length // BLOCK

    def to_blocks(tensor):
        return tensor.reshape(head_count, blocks, BLOCK, tensor.shape[-1]).transpose(1, 0, 2, 3)

    lower_mask = jnp.tril(jnp.ones((BLOCK, BLOCK), dtype=bool))[:, :, None]

    def advance(state_stack, pieces):
        query_block, key_block, value_block, g_blk = pieces
        cumulative_log = jnp.cumsum(g_blk, axis=1)
        across_blocks = jnp.einsum(
            "bqy,byo->bqo",
            query_block * jnp.exp(cumulative_log),
            state_stack,
            precision=highest_precision,
        )
        spread = cumulative_log[:, :, None, :] - cumulative_log[:, None, :, :]
        decays = jnp.where(lower_mask, jnp.exp(jnp.where(lower_mask, spread, 0.0)), 0.0)
        scores = jnp.einsum(
            "hik,hijk->hij",
            query_block,
            decays * key_block[:, None, :, :],
            precision=highest_precision,
        )
        inside = jnp.einsum("hij,hjv->hiv", scores, value_block, precision=highest_precision)
        final_log_decay = cumulative_log[:, -1:, :]
        carried = jnp.exp(final_log_decay[:, 0, :])[..., None] * state_stack
        fresh_portion = jnp.einsum(
            "moc,moa->mca",
            key_block * jnp.exp(final_log_decay - cumulative_log),
            value_block,
            precision=highest_precision,
        )
        return (carried + fresh_portion, across_blocks + inside)

    start_state = jnp.zeros((head_count, key_dim, values.shape[-1]), jnp.float32)
    final_state, outputs = lax.scan(
        advance,
        start_state,
        (to_blocks(queries), to_blocks(taken), to_blocks(values), to_blocks(kept_log)),
    )
    return (
        outputs.transpose(1, 0, 2, 3).reshape(head_count, length, values.shape[-1]),
        final_state,
    )


def key_width(row_count):
    for candidate in range(min(row_count, 1024), 0, -1):
        if row_count % candidate == 0:
            return candidate
    return 1


def spread_shards(
    inputs,
    norm_gain,
    hg_query_w,
    hg_fwd_w,
    hg_bwd_w,
    hg_value_w,
    floor_gap,
    hg_norm_gain,
    df_query_w,
    df_key_w,
    df_value_w,
    diff_lambda,
    df_norm_gain,
    out_hg_w,
    out_df_w,
    post_gain,
):
    tok_rows = inputs[0]
    length = tok_rows.shape[0]
    rows_float = tok_rows.astype(jnp.float32)
    normed = (rows_float * rms_scale(rows_float) * norm_gain).astype(jnp.bfloat16)
    pieces = (
        lax.all_gather(hg_query_w, ("sp", "fs"), axis=0, tiled=True),
        lax.all_gather(hg_fwd_w, ("sp", "fs"), axis=0, tiled=True),
        lax.all_gather(hg_bwd_w, ("sp", "fs"), axis=0, tiled=True),
        lax.all_gather(hg_value_w, ("sp", "fs"), axis=0, tiled=True),
        lax.all_gather(df_query_w, ("sp", "fs"), axis=0, tiled=True),
        lax.all_gather(df_key_w, ("sp", "fs"), axis=0, tiled=True),
        lax.all_gather(df_value_w, ("sp", "fs"), axis=0, tiled=True),
    )
    summed = tuple((jnp.dot(normed, piece, preferred_element_type=jnp.float32) for piece in pieces))
    hg_query, hg_fwd, hg_bwd, hg_value, df_query, df_key, df_value = [
        member.astype(jnp.bfloat16) for member in summed
    ]
    heads_hg = hg_query.shape[1] // HEAD

    def split_heads(tensor):
        return tensor.astype(jnp.float32).reshape(length, heads_hg, HEAD).transpose(1, 0, 2)

    queries = jax.nn.silu(split_heads(hg_query))
    values = split_heads(hg_value)

    def summarize(raw_gate, gap_row, flipped):
        taken = gap_row.reshape(heads_hg, 1, HEAD) * jax.nn.sigmoid(-split_heads(raw_gate))
        series = (queries, taken, values, jnp.log1p(-taken))
        if flipped:
            series = tuple((jnp.flip(tensor, axis=1) for tensor in series))
        local_out, final_state = span_scan(*series)
        cumulative_log = jnp.cumsum(series[3], axis=1)
        return (
            local_out,
            final_state,
            jnp.exp(cumulative_log[:, -1, :]),
            series[0] * jnp.exp(cumulative_log),
        )

    forward_output, fwd_state, fwd_decay, forward_reader = summarize(hg_fwd, floor_gap[0], False)
    backward_output, bwd_state, bwd_decay, backward_reader = summarize(hg_bwd, floor_gap[1], True)
    all_decay, all_state = (
        lax.all_gather(
            jnp.stack([fwd_decay, bwd_decay])[None].astype(jnp.bfloat16), "sp", axis=0, tiled=True
        ).astype(jnp.float32),
        lax.all_gather(
            jnp.stack([fwd_state, bwd_state])[None].astype(jnp.bfloat16), "sp", axis=0, tiled=True
        ).astype(jnp.float32),
    )
    position = lax.axis_index("sp")
    members = all_decay.shape[0]

    def forward_step(member, running):
        joined = all_decay[member, 0][..., None] * running + all_state[member, 0]
        return jnp.where(member < position, joined, running)

    def backward_step(offset, running):
        member = members - 1 - offset
        joined = all_decay[member, 1][..., None] * running + all_state[member, 1]
        return jnp.where(member > position, joined, running)

    forward_carry = lax.fori_loop(0, members, forward_step, jnp.zeros_like(fwd_state))
    backward_carry = lax.fori_loop(0, members, backward_step, jnp.zeros_like(bwd_state))
    forward_sum = forward_output + jnp.einsum(
        "bqy,byo->bqo", forward_reader, forward_carry, precision=highest_precision
    )
    bwd_total = jnp.flip(
        backward_output
        + jnp.einsum("bqy,byo->bqo", backward_reader, backward_carry, precision=highest_precision),
        axis=1,
    )
    recurrent = forward_sum + bwd_total
    hg_out = (
        (recurrent * rms_scale(recurrent) * hg_norm_gain)
        .transpose(1, 0, 2)
        .reshape(length, heads_hg * HEAD)
        .astype(jnp.bfloat16)
    )
    heads_df = df_value.shape[1] // DFV
    df_queries = df_query.reshape(length, heads_df, 2, DQK)
    score_scale = DQK ** (-0.5)
    start_carry = (
        jnp.full((heads_df, 2, length), -1e30, jnp.float32),
        jnp.zeros((heads_df, 2, length), jnp.float32),
        jnp.zeros((heads_df, 2, length, DFV), jnp.float32),
    )
    carry = start_carry
    key_rows = lax.all_gather(df_key, "sp", axis=0, tiled=True)
    value_rows = lax.all_gather(df_value, "sp", axis=0, tiled=True)
    row_count = key_rows.shape[0]
    block_rows = key_width(row_count)
    key_blocks = key_rows.reshape(row_count // block_rows, block_rows, heads_df, 2, DQK)
    value_blocks = value_rows.reshape(row_count // block_rows, block_rows, heads_df, DFV)

    def key_step(running, block_pair):
        tops, totals, accums = running
        key_blk, value_blk = block_pair
        scores = (
            jnp.einsum("qhmd,khmd->hmqk", df_queries, key_blk, preferred_element_type=jnp.float32)
            * score_scale
        )
        new_tops = jnp.maximum(tops, jnp.max(scores, axis=-1))
        factor = jnp.exp(tops - new_tops)
        weights_blk = jnp.exp(scores - new_tops[..., None])
        totals = totals * factor + jnp.sum(weights_blk, axis=-1)
        accums = accums * factor[..., None] + jnp.einsum(
            "hmqk,khd->hmqd",
            weights_blk.astype(jnp.bfloat16),
            value_blk,
            preferred_element_type=jnp.float32,
        )
        return ((new_tops, totals, accums), None)

    carry, unused = lax.scan(key_step, carry, (key_blocks, value_blocks))
    tops, totals, accums = carry
    maps = accums / totals[..., None]
    weighted = maps[:, 0] - diff_lambda[:, None, None] * maps[:, 1]
    df_out = (
        (weighted * rms_scale(weighted) * df_norm_gain * df_factor)
        .transpose(1, 0, 2)
        .reshape(length, heads_df * DFV)
        .astype(jnp.bfloat16)
    )
    mixture = lax.psum_scatter(
        (
            jnp.dot(hg_out, out_hg_w, preferred_element_type=jnp.float32)
            + jnp.dot(df_out, out_df_w, preferred_element_type=jnp.float32)
        ).astype(jnp.bfloat16),
        "tp",
        scatter_dimension=0,
        tiled=True,
    ).astype(jnp.float32)
    return (mixture * rms_scale(mixture) * post_gain).astype(jnp.bfloat16)[None]


MESH = pl.DeviceIdType.MESH
VMEM_SPEC = pl.BlockSpec(memory_space=pltpu.VMEM)
ANY_SPEC = pl.BlockSpec(memory_space=pl.ANY)
STEEPEST = -math.log1p(-0.1)


def greet(peers):
    barrier = pltpu.get_barrier_semaphore()
    for peer in peers:
        pl.semaphore_signal(barrier, inc=1, device_id=peer, device_id_type=MESH)
    pl.semaphore_wait(barrier, len(peers))


def gather_kernel(n_sp, n_fs, wp_ref, x_ref, wg_ref, xg_ref, own_sem, s1, r1, sx, rx, s2, r2):
    sp, fs = lax.axis_index("sp"), lax.axis_index("fs")
    sp_peers = [lax.rem(sp + d, n_sp) for d in range(1, n_sp)]
    fs_peers = [lax.rem(fs + e, n_fs) for e in range(1, n_fs)]
    greet([{"sp": p} for p in sp_peers] + [{"fs": p} for p in fs_peers])

    def remote(src, dst, send, recv, peer):
        return pltpu.make_async_remote_copy(
            src_ref=src, dst_ref=dst, send_sem=send, recv_sem=recv, device_id=peer, device_id_type=MESH
        )

    started = []
    along = []
    for d, peer in enumerate(sp_peers):
        copy = remote(wp_ref.at[peer], wg_ref.at[sp, fs], s1.at[d], r1.at[d], {"sp": peer})
        copy.start()
        along.append(copy)
    for e, peer in enumerate(fs_peers):
        copy = remote(wp_ref.at[sp], wg_ref.at[sp, fs], s2.at[0, e], r2.at[0, e], {"fs": peer})
        copy.start()
        started.append(copy)
    for d, peer in enumerate(sp_peers):
        copy = remote(x_ref, xg_ref.at[sp], sx.at[d], rx.at[d], {"sp": peer})
        copy.start()
        started.append(copy)
    own_w = pltpu.make_async_copy(wp_ref.at[sp], wg_ref.at[sp, fs], own_sem.at[0])
    own_x = pltpu.make_async_copy(x_ref, xg_ref.at[sp], own_sem.at[1])
    own_w.start()
    own_x.start()
    for d in range(n_sp - 1):
        along[d].wait_recv()
        source = lax.rem(sp + n_sp - d - 1, n_sp)
        for e, peer in enumerate(fs_peers):
            piece = wg_ref.at[source, fs]
            copy = remote(piece, piece, s2.at[d + 1, e], r2.at[d + 1, e], {"fs": peer})
            copy.start()
            started.append(copy)
    own_w.wait()
    own_x.wait()
    for copy in along:
        copy.wait_send()
    for copy in started:
        copy.wait()


def mixer_kernel(
    hr, ha, x_ref, w_ref, gain_ref, gap_ref, hgain_ref, lam_ref, dgain_ref, o_ref, proj_ref
):
    length = x_ref.shape[0]
    rows = min(length, 128)
    for start in range(0, length, rows):
        x = x_ref[start : start + rows, :].astype(jnp.float32)
        scale = lax.rsqrt(jnp.mean(x * x, axis=-1, keepdims=True) + epsilon)
        normed = (x * scale * gain_ref[...]).astype(jnp.bfloat16)
        proj_ref[start : start + rows, :] = jnp.dot(
            normed, w_ref[...], preferred_element_type=jnp.float32
        ).astype(jnp.bfloat16)
    wide = hr * HEAD
    hq = proj_ref[:, 0:wide].astype(jnp.float32)
    hf = proj_ref[:, wide : 2 * wide].astype(jnp.float32)
    hb = proj_ref[:, 2 * wide : 3 * wide].astype(jnp.float32)
    hv = proj_ref[:, 3 * wide : 4 * wide]
    queries = hq * jax.nn.sigmoid(hq)
    taken_f = gap_ref[0:1, :] * jax.nn.sigmoid(-hf)
    taken_b = gap_ref[1:2, :] * jax.nn.sigmoid(-hb)
    kept_b = jnp.log1p(-taken_b)
    kept = jnp.concatenate([jnp.log1p(-taken_f), kept_b], axis=1)
    row = lax.broadcasted_iota(jnp.int32, (length, length), 0)
    col = lax.broadcasted_iota(jnp.int32, (length, length), 1)
    lower = row >= col
    upper = row <= col
    ones = jnp.where(lower, 1.0, 0.0).astype(jnp.bfloat16)
    cumulative = jnp.zeros_like(kept)
    rest = kept
    for _ in range(3):
        part = rest.astype(jnp.bfloat16)
        rest = rest - part.astype(jnp.float32)
        cumulative = cumulative + jnp.dot(ones, part, preferred_element_type=jnp.float32)
    before = cumulative[:, wide:] - kept_b
    after = cumulative[:, :wide]
    after = after - 0.5 * after[length - 1 : length, :]
    before = before - 0.5 * before[length - 1 : length, :]
    qf = (queries * jnp.exp(after)).astype(jnp.bfloat16)
    kf = (taken_f * jnp.exp(-after)).astype(jnp.bfloat16)
    qb = (queries * jnp.exp(-before)).astype(jnp.bfloat16)
    kb = (taken_b * jnp.exp(before)).astype(jnp.bfloat16)
    across = (((1,), (1,)), ((), ()))
    for h in range(hr):
        span = slice(h * HEAD, (h + 1) * HEAD)
        fwd = lax.dot_general(qf[:, span], kf[:, span], across, preferred_element_type=jnp.float32)
        bwd = lax.dot_general(qb[:, span], kb[:, span], across, preferred_element_type=jnp.float32)
        scores = jnp.where(lower, fwd, 0.0) + jnp.where(upper, bwd, 0.0)
        out = jnp.dot(scores.astype(jnp.bfloat16), hv[:, span], preferred_element_type=jnp.float32)
        scale = lax.rsqrt(jnp.mean(out * out, axis=-1, keepdims=True) + epsilon)
        o_ref[:, span] = (out * scale * hgain_ref[...]).astype(jnp.bfloat16)
    q_at = 4 * wide
    k_at = q_at + ha * 2 * DQK
    v_at = k_at + ha * 2 * DQK
    for h in range(ha):
        value = proj_ref[:, v_at + h * DFV : v_at + (h + 1) * DFV]
        maps = []
        for m in range(2):
            offset = (h * 2 + m) * DQK
            query = proj_ref[:, q_at + offset : q_at + offset + DQK]
            key = proj_ref[:, k_at + offset : k_at + offset + DQK]
            scores = lax.dot_general(
                query, key, across, preferred_element_type=jnp.float32
            ) * (DQK ** (-0.5))
            shifted = jnp.exp(scores - jnp.max(scores, axis=-1, keepdims=True))
            total = jnp.sum(shifted, axis=-1, keepdims=True)
            accum = jnp.dot(shifted.astype(jnp.bfloat16), value, preferred_element_type=jnp.float32)
            maps.append(accum / total)
        weighted = maps[0] - lam_ref[h] * maps[1]
        scale = lax.rsqrt(jnp.mean(weighted * weighted, axis=-1, keepdims=True) + epsilon)
        o_ref[:, wide + h * DFV : wide + (h + 1) * DFV] = (
            weighted * scale * dgain_ref[...] * df_factor
        ).astype(jnp.bfloat16)


def output_kernel(
    n_sp, n_tp, wide, o_ref, wh_ref, wd_ref, gain_ref, out_ref, og, pbuf, rbuf, s1, r1, s2, r2
):
    sp, tp = lax.axis_index("sp"), lax.axis_index("tp")
    sp_peers = [lax.rem(sp + d, n_sp) for d in range(1, n_sp)]
    tp_peers = [lax.rem(tp + d, n_tp) for d in range(1, n_tp)]
    greet([{"sp": p} for p in sp_peers] + [{"tp": p} for p in tp_peers])
    copies = []
    for d, peer in enumerate(sp_peers):
        copy = pltpu.make_async_remote_copy(
            src_ref=o_ref.at[peer],
            dst_ref=og.at[sp],
            send_sem=s1.at[d],
            recv_sem=r1.at[d],
            device_id={"sp": peer},
            device_id_type=MESH,
        )
        copy.start()
        copies.append(copy)
    og[sp] = o_ref[sp]
    for copy in copies:
        copy.wait()
    hg = jnp.concatenate([og[s, :, :wide] for s in range(n_sp)], axis=1)
    df = jnp.concatenate([og[s, :, wide:] for s in range(n_sp)], axis=1)
    partial = jnp.dot(hg, wh_ref[...], preferred_element_type=jnp.float32) + jnp.dot(
        df, wd_ref[...], preferred_element_type=jnp.float32
    )
    pbuf[...] = partial.astype(jnp.bfloat16).reshape(pbuf.shape)
    copies = []
    for d, peer in enumerate(tp_peers):
        copy = pltpu.make_async_remote_copy(
            src_ref=pbuf.at[peer],
            dst_ref=rbuf.at[d],
            send_sem=s2.at[d],
            recv_sem=r2.at[d],
            device_id={"tp": peer},
            device_id_type=MESH,
        )
        copy.start()
        copies.append(copy)
    mixture = pbuf[tp].astype(jnp.float32)
    for d, copy in enumerate(copies):
        copy.wait()
        mixture = mixture + rbuf[d].astype(jnp.float32)
    scale = lax.rsqrt(jnp.mean(mixture * mixture, axis=-1, keepdims=True) + epsilon)
    out_ref[...] = (mixture * scale * gain_ref[...]).astype(jnp.bfloat16)


def headwise_shards(
    n_sp,
    n_fs,
    n_tp,
    inputs,
    norm_gain,
    hg_query_w,
    hg_fwd_w,
    hg_bwd_w,
    hg_value_w,
    floor_gap,
    hg_norm_gain,
    df_query_w,
    df_key_w,
    df_value_w,
    diff_lambda,
    df_norm_gain,
    out_hg_w,
    out_df_w,
    post_gain,
):
    x = inputs[0]
    tokens, depth = x.shape
    length = tokens * n_sp
    k_rows = hg_query_w.shape[0]
    hr = hg_query_w.shape[1] // HEAD // n_sp
    ha = df_value_w.shape[1] // DFV // n_sp
    wide = hr * HEAD
    out_wide = wide + ha * DFV
    pieces = [hg_query_w, hg_fwd_w, hg_bwd_w, hg_value_w, df_query_w, df_key_w, df_value_w]
    packed = jnp.concatenate(
        [w.reshape(k_rows, n_sp, w.shape[1] // n_sp) for w in pieces], axis=2
    ).transpose(1, 0, 2)
    columns = packed.shape[2]
    dma = pltpu.SemaphoreType.DMA
    weights, rows = pl.pallas_call(
        functools.partial(gather_kernel, n_sp, n_fs),
        out_shape=(
            jax.ShapeDtypeStruct((n_sp, n_fs, k_rows, columns), jnp.bfloat16),
            jax.ShapeDtypeStruct((n_sp, tokens, depth), jnp.bfloat16),
        ),
        in_specs=[VMEM_SPEC, VMEM_SPEC],
        out_specs=(VMEM_SPEC, VMEM_SPEC),
        scratch_shapes=[
            dma((2,)),
            dma((n_sp - 1,)),
            dma((n_sp - 1,)),
            dma((n_sp - 1,)),
            dma((n_sp - 1,)),
            dma((n_sp, n_fs - 1)),
            dma((n_sp, n_fs - 1)),
        ],
        compiler_params=pltpu.CompilerParams(collective_id=0, has_side_effects=True),
        name="gather",
    )(packed, x)
    position = lax.axis_index("sp")
    gap = lax.dynamic_slice_in_dim(floor_gap, position * wide, wide, axis=1)
    lam = lax.dynamic_slice_in_dim(diff_lambda, position * ha, ha, axis=0)
    mixed_heads = pl.pallas_call(
        functools.partial(mixer_kernel, hr, ha),
        out_shape=jax.ShapeDtypeStruct((length, out_wide), jnp.bfloat16),
        in_specs=[VMEM_SPEC] * 5 + [pl.BlockSpec(memory_space=pltpu.SMEM), VMEM_SPEC],
        out_specs=VMEM_SPEC,
        scratch_shapes=[pltpu.VMEM((length, columns), jnp.bfloat16)],
        name="mixer",
    )(
        rows.reshape(length, depth),
        weights.reshape(n_sp * n_fs * k_rows, columns),
        norm_gain[None],
        gap,
        hg_norm_gain[None],
        lam,
        df_norm_gain[None],
    )
    own_rows = tokens // n_tp
    out = pl.pallas_call(
        functools.partial(output_kernel, n_sp, n_tp, wide),
        out_shape=jax.ShapeDtypeStruct((own_rows, depth), jnp.bfloat16),
        in_specs=[VMEM_SPEC] * 4,
        out_specs=VMEM_SPEC,
        scratch_shapes=[
            pltpu.VMEM((n_sp, tokens, out_wide), jnp.bfloat16),
            pltpu.VMEM((n_tp, own_rows, depth), jnp.bfloat16),
            pltpu.VMEM((max(n_tp - 1, 1), own_rows, depth), jnp.bfloat16),
            dma((n_sp - 1,)),
            dma((n_sp - 1,)),
            dma((max(n_tp - 1, 1),)),
            dma((max(n_tp - 1, 1),)),
        ],
        compiler_params=pltpu.CompilerParams(collective_id=1, has_side_effects=True),
        name="output",
    )(mixed_heads.reshape(n_sp, tokens, out_wide), out_hg_w, out_df_w, post_gain[None])
    return out[None]


def shards(n_sp, n_fs, n_tp, *arrays):
    inputs, hg_query_w, df_value_w = arrays[0], arrays[2], arrays[10]
    heads_hg = hg_query_w.shape[1] // HEAD
    heads_df = df_value_w.shape[1] // DFV
    length = inputs.shape[1] * n_sp
    if heads_hg % n_sp == 0 and heads_df % n_sp == 0 and length * STEEPEST < 60.0:
        return headwise_shards(n_sp, n_fs, n_tp, *arrays)
    return spread_shards(*arrays)


def solution(mesh):
    sizes = [mesh.shape[name] for name in ("sp", "fs", "tp")]
    in_specs = (
        P("fs", "sp", None),
        P(),
        P(("sp", "fs"), "tp"),
        P(("sp", "fs"), "tp"),
        P(("sp", "fs"), "tp"),
        P(("sp", "fs"), "tp"),
        P(None, "tp"),
        P(),
        P(("sp", "fs"), "tp"),
        P(("sp", "fs"), "tp"),
        P(("sp", "fs"), "tp"),
        P("tp"),
        P(),
        P("tp", None),
        P("tp", None),
        P(),
    )
    out_specs = P("fs", ("sp", "tp"), None)
    return jax.shard_map(functools.partial(shards, *sizes), mesh=mesh, in_specs=in_specs, out_specs=out_specs, check_vma=False)
```

```python
import functools
import math

import jax
import jax.numpy as jnp
from jax import lax
from jax.experimental import pallas as pl
from jax.experimental.pallas import tpu as pltpu
from jax.sharding import PartitionSpec as P

HEAD = 64
DQK = 32
BLOCK = 64
DFV = 64


epsilon = 1e-06
df_factor = 0.8
highest_precision = lax.Precision.HIGHEST


def rms_scale(values):
    return lax.rsqrt(jnp.mean(values * values, axis=-1, keepdims=True) + epsilon)


def span_scan(queries, taken, values, kept_log):
    head_count, length, key_dim = queries.shape
    blocks = length // BLOCK

    def to_blocks(tensor):
        return tensor.reshape(head_count, blocks, BLOCK, tensor.shape[-1]).transpose(1, 0, 2, 3)

    lower_mask = jnp.tril(jnp.ones((BLOCK, BLOCK), dtype=bool))[:, :, None]

    def advance(state_stack, pieces):
        query_block, key_block, value_block, g_blk = pieces
        cumulative_log = jnp.cumsum(g_blk, axis=1)
        across_blocks = jnp.einsum(
            "bqy,byo->bqo",
            query_block * jnp.exp(cumulative_log),
            state_stack,
            precision=highest_precision,
        )
        spread = cumulative_log[:, :, None, :] - cumulative_log[:, None, :, :]
        decays = jnp.where(lower_mask, jnp.exp(jnp.where(lower_mask, spread, 0.0)), 0.0)
        scores = jnp.einsum(
            "hik,hijk->hij",
            query_block,
            decays * key_block[:, None, :, :],
            precision=highest_precision,
        )
        inside = jnp.einsum("hij,hjv->hiv", scores, value_block, precision=highest_precision)
        final_log_decay = cumulative_log[:, -1:, :]
        carried = jnp.exp(final_log_decay[:, 0, :])[..., None] * state_stack
        fresh_portion = jnp.einsum(
            "moc,moa->mca",
            key_block * jnp.exp(final_log_decay - cumulative_log),
            value_block,
            precision=highest_precision,
        )
        return (carried + fresh_portion, across_blocks + inside)

    start_state = jnp.zeros((head_count, key_dim, values.shape[-1]), jnp.float32)
    final_state, outputs = lax.scan(
        advance,
        start_state,
        (to_blocks(queries), to_blocks(taken), to_blocks(values), to_blocks(kept_log)),
    )
    return (
        outputs.transpose(1, 0, 2, 3).reshape(head_count, length, values.shape[-1]),
        final_state,
    )


def key_width(row_count):
    for candidate in range(min(row_count, 1024), 0, -1):
        if row_count % candidate == 0:
            return candidate
    return 1


def spread_shards(
    inputs,
    norm_gain,
    hg_query_w,
    hg_fwd_w,
    hg_bwd_w,
    hg_value_w,
    floor_gap,
    hg_norm_gain,
    df_query_w,
    df_key_w,
    df_value_w,
    diff_lambda,
    df_norm_gain,
    out_hg_w,
    out_df_w,
    post_gain,
):
    tok_rows = inputs[0]
    length = tok_rows.shape[0]
    rows_float = tok_rows.astype(jnp.float32)
    normed = (rows_float * rms_scale(rows_float) * norm_gain).astype(jnp.bfloat16)
    pieces = (
        lax.all_gather(hg_query_w, ("sp", "fs"), axis=0, tiled=True),
        lax.all_gather(hg_fwd_w, ("sp", "fs"), axis=0, tiled=True),
        lax.all_gather(hg_bwd_w, ("sp", "fs"), axis=0, tiled=True),
        lax.all_gather(hg_value_w, ("sp", "fs"), axis=0, tiled=True),
        lax.all_gather(df_query_w, ("sp", "fs"), axis=0, tiled=True),
        lax.all_gather(df_key_w, ("sp", "fs"), axis=0, tiled=True),
        lax.all_gather(df_value_w, ("sp", "fs"), axis=0, tiled=True),
    )
    summed = tuple((jnp.dot(normed, piece, preferred_element_type=jnp.float32) for piece in pieces))
    hg_query, hg_fwd, hg_bwd, hg_value, df_query, df_key, df_value = [
        member.astype(jnp.bfloat16) for member in summed
    ]
    heads_hg = hg_query.shape[1] // HEAD

    def split_heads(tensor):
        return tensor.astype(jnp.float32).reshape(length, heads_hg, HEAD).transpose(1, 0, 2)

    queries = jax.nn.silu(split_heads(hg_query))
    values = split_heads(hg_value)

    def summarize(raw_gate, gap_row, flipped):
        taken = gap_row.reshape(heads_hg, 1, HEAD) * jax.nn.sigmoid(-split_heads(raw_gate))
        series = (queries, taken, values, jnp.log1p(-taken))
        if flipped:
            series = tuple((jnp.flip(tensor, axis=1) for tensor in series))
        local_out, final_state = span_scan(*series)
        cumulative_log = jnp.cumsum(series[3], axis=1)
        return (
            local_out,
            final_state,
            jnp.exp(cumulative_log[:, -1, :]),
            series[0] * jnp.exp(cumulative_log),
        )

    forward_output, fwd_state, fwd_decay, forward_reader = summarize(hg_fwd, floor_gap[0], False)
    backward_output, bwd_state, bwd_decay, backward_reader = summarize(hg_bwd, floor_gap[1], True)
    all_decay, all_state = (
        lax.all_gather(
            jnp.stack([fwd_decay, bwd_decay])[None].astype(jnp.bfloat16), "sp", axis=0, tiled=True
        ).astype(jnp.float32),
        lax.all_gather(
            jnp.stack([fwd_state, bwd_state])[None].astype(jnp.bfloat16), "sp", axis=0, tiled=True
        ).astype(jnp.float32),
    )
    position = lax.axis_index("sp")
    members = all_decay.shape[0]

    def forward_step(member, running):
        joined = all_decay[member, 0][..., None] * running + all_state[member, 0]
        return jnp.where(member < position, joined, running)

    def backward_step(offset, running):
        member = members - 1 - offset
        joined = all_decay[member, 1][..., None] * running + all_state[member, 1]
        return jnp.where(member > position, joined, running)

    forward_carry = lax.fori_loop(0, members, forward_step, jnp.zeros_like(fwd_state))
    backward_carry = lax.fori_loop(0, members, backward_step, jnp.zeros_like(bwd_state))
    forward_sum = forward_output + jnp.einsum(
        "bqy,byo->bqo", forward_reader, forward_carry, precision=highest_precision
    )
    bwd_total = jnp.flip(
        backward_output
        + jnp.einsum("bqy,byo->bqo", backward_reader, backward_carry, precision=highest_precision),
        axis=1,
    )
    recurrent = forward_sum + bwd_total
    hg_out = (
        (recurrent * rms_scale(recurrent) * hg_norm_gain)
        .transpose(1, 0, 2)
        .reshape(length, heads_hg * HEAD)
        .astype(jnp.bfloat16)
    )
    heads_df = df_value.shape[1] // DFV
    df_queries = df_query.reshape(length, heads_df, 2, DQK)
    score_scale = DQK ** (-0.5)
    start_carry = (
        jnp.full((heads_df, 2, length), -1e30, jnp.float32),
        jnp.zeros((heads_df, 2, length), jnp.float32),
        jnp.zeros((heads_df, 2, length, DFV), jnp.float32),
    )
    carry = start_carry
    key_rows = lax.all_gather(df_key, "sp", axis=0, tiled=True)
    value_rows = lax.all_gather(df_value, "sp", axis=0, tiled=True)
    row_count = key_rows.shape[0]
    block_rows = key_width(row_count)
    key_blocks = key_rows.reshape(row_count // block_rows, block_rows, heads_df, 2, DQK)
    value_blocks = value_rows.reshape(row_count // block_rows, block_rows, heads_df, DFV)

    def key_step(running, block_pair):
        tops, totals, accums = running
        key_blk, value_blk = block_pair
        scores = (
            jnp.einsum("qhmd,khmd->hmqk", df_queries, key_blk, preferred_element_type=jnp.float32)
            * score_scale
        )
        new_tops = jnp.maximum(tops, jnp.max(scores, axis=-1))
        factor = jnp.exp(tops - new_tops)
        weights_blk = jnp.exp(scores - new_tops[..., None])
        totals = totals * factor + jnp.sum(weights_blk, axis=-1)
        accums = accums * factor[..., None] + jnp.einsum(
            "hmqk,khd->hmqd",
            weights_blk.astype(jnp.bfloat16),
            value_blk,
            preferred_element_type=jnp.float32,
        )
        return ((new_tops, totals, accums), None)

    carry, unused = lax.scan(key_step, carry, (key_blocks, value_blocks))
    tops, totals, accums = carry
    maps = accums / totals[..., None]
    weighted = maps[:, 0] - diff_lambda[:, None, None] * maps[:, 1]
    df_out = (
        (weighted * rms_scale(weighted) * df_norm_gain * df_factor)
        .transpose(1, 0, 2)
        .reshape(length, heads_df * DFV)
        .astype(jnp.bfloat16)
    )
    mixture = lax.psum_scatter(
        (
            jnp.dot(hg_out, out_hg_w, preferred_element_type=jnp.float32)
            + jnp.dot(df_out, out_df_w, preferred_element_type=jnp.float32)
        ).astype(jnp.bfloat16),
        "tp",
        scatter_dimension=0,
        tiled=True,
    ).astype(jnp.float32)
    return (mixture * rms_scale(mixture) * post_gain).astype(jnp.bfloat16)[None]


MESH = pl.DeviceIdType.MESH
VMEM_SPEC = pl.BlockSpec(memory_space=pltpu.VMEM)
ANY_SPEC = pl.BlockSpec(memory_space=pl.ANY)
STEEPEST = -math.log1p(-0.1)


LANES = 128


def remote(src, dst, send, recv, peer):
    return pltpu.make_async_remote_copy(
        src_ref=src, dst_ref=dst, send_sem=send, recv_sem=recv, device_id=peer, device_id_type=MESH
    )


def recurrence(proj_ref, gap, hgain, hr, store):
    length = proj_ref.shape[0]
    wide = hr * HEAD
    hq = proj_ref[:, 0:wide].astype(jnp.bfloat16).astype(jnp.float32)
    hf = proj_ref[:, wide : 2 * wide].astype(jnp.bfloat16).astype(jnp.float32)
    hb = proj_ref[:, 2 * wide : 3 * wide].astype(jnp.bfloat16).astype(jnp.float32)
    hv = proj_ref[:, 3 * wide : 4 * wide].astype(jnp.bfloat16)
    queries = hq * jax.nn.sigmoid(hq)
    taken_f = gap[0:1, :] * jax.nn.sigmoid(-hf)
    taken_b = gap[1:2, :] * jax.nn.sigmoid(-hb)
    kept_b = jnp.log1p(-taken_b)
    kept = jnp.concatenate([jnp.log1p(-taken_f), kept_b], axis=1)
    row = lax.broadcasted_iota(jnp.int32, (length, length), 0)
    col = lax.broadcasted_iota(jnp.int32, (length, length), 1)
    lower = row >= col
    upper = row <= col
    ones = jnp.where(lower, 1.0, 0.0).astype(jnp.bfloat16)
    cumulative = jnp.zeros_like(kept)
    rest = kept
    for _ in range(3):
        part = rest.astype(jnp.bfloat16)
        rest = rest - part.astype(jnp.float32)
        cumulative = cumulative + jnp.dot(ones, part, preferred_element_type=jnp.float32)
    before = cumulative[:, wide:] - kept_b
    after = cumulative[:, :wide]
    after = after - 0.5 * after[length - 1 : length, :]
    before = before - 0.5 * before[length - 1 : length, :]
    qf = (queries * jnp.exp(after)).astype(jnp.bfloat16)
    kf = (taken_f * jnp.exp(-after)).astype(jnp.bfloat16)
    qb = (queries * jnp.exp(-before)).astype(jnp.bfloat16)
    kb = (taken_b * jnp.exp(before)).astype(jnp.bfloat16)
    across = (((1,), (1,)), ((), ()))
    for h in range(hr):
        span = slice(h * HEAD, (h + 1) * HEAD)
        fwd = lax.dot_general(qf[:, span], kf[:, span], across, preferred_element_type=jnp.float32)
        bwd = lax.dot_general(qb[:, span], kb[:, span], across, preferred_element_type=jnp.float32)
        scores = jnp.where(lower, fwd, 0.0) + jnp.where(upper, bwd, 0.0)
        out = jnp.dot(scores.astype(jnp.bfloat16), hv[:, span], preferred_element_type=jnp.float32)
        scale = lax.rsqrt(jnp.mean(out * out, axis=-1, keepdims=True) + epsilon)
        store(span.start, (out * scale * hgain).astype(jnp.bfloat16))


def attention(proj_ref, first_lam, lam_ref, dgain, q_at, ha, out_at, store):
    across = (((1,), (1,)), ((), ()))
    k_at = q_at + ha * 2 * DQK
    v_at = k_at + ha * 2 * DQK
    for h in range(ha):
        value = proj_ref[:, v_at + h * DFV : v_at + (h + 1) * DFV].astype(jnp.bfloat16)
        maps = []
        for m in range(2):
            offset = (h * 2 + m) * DQK
            query = proj_ref[:, q_at + offset : q_at + offset + DQK].astype(jnp.bfloat16)
            key = proj_ref[:, k_at + offset : k_at + offset + DQK].astype(jnp.bfloat16)
            scores = lax.dot_general(
                query, key, across, preferred_element_type=jnp.float32
            ) * (DQK ** (-0.5))
            shifted = jnp.exp(scores - jnp.max(scores, axis=-1, keepdims=True))
            total = jnp.sum(shifted, axis=-1, keepdims=True)
            accum = jnp.dot(shifted.astype(jnp.bfloat16), value, preferred_element_type=jnp.float32)
            maps.append(accum / total)
        weighted = maps[0] - lam_ref[first_lam + h] * maps[1]
        scale = lax.rsqrt(jnp.mean(weighted * weighted, axis=-1, keepdims=True) + epsilon)
        store(out_at + h * DFV, (weighted * scale * dgain * df_factor).astype(jnp.bfloat16))


def block_kernel(
    n_sp, n_fs, n_tp, hr, ha,
    x_ref, w0, w1, w2, w3, w4, w5, w6, gain_ref, gap_ref, hgain_ref, lam_ref, dgain_ref,
    wh_hbm, wd_hbm, post_ref, out_ref,
    wp, wg, xg, proj, ob, og, pbuf, rbuf, wh, wd,
    local, s1, r1, sx, rx, sy, ry, s2, r2, s3, r3, s4, r4, s5, r5,
):
    sp, fs, tp = lax.axis_index("sp"), lax.axis_index("fs"), lax.axis_index("tp")
    sp_peers = [lax.rem(sp + d, n_sp) for d in range(1, n_sp)]
    sp_froms = [lax.rem(sp + n_sp - d, n_sp) for d in range(1, n_sp)]
    tp_peers = [lax.rem(tp + d, n_tp) for d in range(1, n_tp)]
    tp_froms = [lax.rem(tp + n_tp - d, n_tp) for d in range(1, n_tp)]
    paired = n_fs == 4
    if paired:
        low, high = lax.rem(fs, 2), fs // 2
        fs_peers = [high * 2 + 1 - low, (1 - high) * 2 + low]
        fs_froms = fs_peers
    else:
        fs_peers = [lax.rem(fs + e, n_fs) for e in range(1, n_fs)]
        fs_froms = [lax.rem(fs + n_fs - e, n_fs) for e in range(1, n_fs)]
    barrier = pltpu.get_barrier_semaphore()
    peers = (
        [{"sp": p} for p in sp_peers] + [{"fs": p} for p in fs_peers] + [{"tp": p} for p in tp_peers]
    )
    for peer in peers:
        pl.semaphore_signal(barrier, inc=1, device_id=peer, device_id_type=MESH)
    load_wh = pltpu.make_async_copy(wh_hbm, wh, local.at[0])
    load_wd = pltpu.make_async_copy(wd_hbm, wd, local.at[1])
    tokens, depth = x_ref.shape
    k_rows = w0.shape[0]
    wide = hr * HEAD
    thin = ha * DFV
    half = k_rows // 2
    for s in range(n_sp):
        for b, w in enumerate((w0, w1, w2, w3)):
            wp[s, b * k_rows : (b + 1) * k_rows, :] = w[:, s * wide : (s + 1) * wide]
        cut = slice(s * thin, (s + 1) * thin)
        wp[s, 4 * k_rows : 5 * k_rows, :] = jnp.concatenate([w4[:, cut], w5[:, cut]], axis=1)
        wp[s, 5 * k_rows :, :] = jnp.concatenate([w6[:half, cut], w6[half:, cut]], axis=1)
    pl.semaphore_wait(barrier, len(peers))

    started = []

    def send(*args):
        copy = remote(*args)
        copy.start()
        started.append(copy)
        return copy

    along = [
        send(wp.at[peer], wg.at[sp, fs], s1.at[d], r1.at[d], {"sp": peer})
        for d, peer in enumerate(sp_peers)
    ]
    across_fs = [
        [
            send(wp.at[sp], wg.at[sp, fs], s2.at[0, e], r2.at[0, e], {"fs": peer})
            for e, peer in enumerate(fs_peers)
        ]
    ]
    share = tokens // n_tp
    mine = pl.ds(pl.multiple_of(tp * share, share), share)
    rows_in = [
        send(x_ref.at[mine, :], xg.at[sp, mine, :], sx.at[d], rx.at[d], {"sp": peer})
        for d, peer in enumerate(sp_peers)
    ]
    load_wh.start()
    load_wd.start()

    piece_rows = wp.shape[1]
    cuts = (slice(0, piece_rows // 2), slice(piece_rows // 2, piece_rows))
    relays = []

    def spread(k):
        along[k - 1].wait_recv()
        piece = wg.at[sp_froms[k - 1], fs]
        across_fs.append(
            [
                send(piece, piece, s2.at[k, e], r2.at[k, e], {"fs": peer})
                for e, peer in enumerate(fs_peers)
            ]
        )

    def relay(k):
        source = sp if k == 0 else sp_froms[k - 1]
        for e, copy in enumerate(across_fs[k]):
            copy.wait_recv()
            if paired:
                piece = wg.at[source, fs_peers[e], cuts[e], :]
                relays.append(
                    (k, send(piece, piece, s5.at[k, e], r5.at[k, e], {"fs": fs_peers[1 - e]}))
                )

    def normalize(s, rows):
        x = rows.astype(jnp.float32)
        scale = lax.rsqrt(jnp.mean(x * x, axis=-1, keepdims=True) + epsilon)
        xg[s] = (x * scale * gain_ref[...]).astype(jnp.bfloat16)

    wg[sp, fs] = wp[sp]
    for k in range(1, n_sp):
        spread(k)
        relay(k - 1)
    normalize(sp, x_ref[...])
    handed = []
    for d in range(n_sp - 1):
        rows_in[d].wait_recv()
        part = xg.at[sp_froms[d], mine, :]
        handed.append(
            [
                send(part, part, sy.at[d, e], ry.at[d, e], {"tp": peer})
                for e, peer in enumerate(tp_peers)
            ]
        )
    relay(n_sp - 1)
    for d in range(n_sp - 1):
        for copy in handed[d]:
            copy.wait()
        normalize(sp_froms[d], xg[sp_froms[d]])

    def project(k):
        source = sp if k == 0 else sp_froms[k - 1]
        for at, copy in relays:
            if at == k:
                copy.wait_recv()
        blocks = [
            jnp.concatenate(
                [wg[source, f, b * k_rows : (b + 1) * k_rows, :] for f in range(n_fs)], axis=0
            )
            for b in range(5)
        ]
        last = []
        for f in range(n_fs):
            tail = wg[source, f, 5 * k_rows :, :]
            last += [tail[:, :thin], tail[:, thin:]]
        weights = jnp.concatenate(blocks + [jnp.concatenate(last, axis=0)], axis=1)
        span = pl.ds(pl.multiple_of(source * (n_fs * k_rows), LANES), n_fs * k_rows)
        for s in range(n_sp):
            here = slice(s * tokens, (s + 1) * tokens)
            added = jnp.dot(xg[s, :, span], weights, preferred_element_type=jnp.float32)
            if k == 0:
                proj[here, :] = added
            else:
                proj[here, :] += added

    for k in range(n_sp):
        project(k)

    def store(at, block):
        width = block.shape[1]
        for s in range(n_sp):
            ob[s, :, at : at + width] = block[s * tokens : (s + 1) * tokens]

    gap = gap_ref[:, pl.ds(pl.multiple_of(sp * wide, LANES), wide)]
    recurrence(proj, gap, hgain_ref[...], hr, store)
    attention(proj, sp * ha, lam_ref, dgain_ref[...], 4 * wide, ha, wide, store)

    heads = [
        send(ob.at[peer], og.at[sp], s3.at[d], r3.at[d], {"sp": peer})
        for d, peer in enumerate(sp_peers)
    ]
    og[sp] = ob[sp]
    load_wh.wait()
    load_wd.wait()
    for copy in heads:
        copy.wait_recv()
    hg = jnp.concatenate([og[s, :, :wide] for s in range(n_sp)], axis=1)
    df = jnp.concatenate([og[s, :, wide:] for s in range(n_sp)], axis=1)
    partial = jnp.dot(hg, wh[...], preferred_element_type=jnp.float32) + jnp.dot(
        df, wd[...], preferred_element_type=jnp.float32
    )
    pbuf[...] = partial.astype(jnp.bfloat16).reshape(pbuf.shape)
    sums = [
        send(pbuf.at[peer], rbuf.at[d], s4.at[d], r4.at[d], {"tp": peer})
        for d, peer in enumerate(tp_peers)
    ]
    mixture = pbuf[tp].astype(jnp.float32)
    for d, copy in enumerate(sums):
        copy.wait_recv()
        mixture = mixture + rbuf[d].astype(jnp.float32)
    scale = lax.rsqrt(jnp.mean(mixture * mixture, axis=-1, keepdims=True) + epsilon)
    out_ref[...] = (mixture * scale * post_ref[...]).astype(jnp.bfloat16)
    waited = {id(copy) for group in handed for copy in group}
    for copy in started:
        if id(copy) not in waited:
            copy.wait_send()


def headwise_shards(
    n_sp, n_fs, n_tp,
    inputs, norm_gain, hg_query_w, hg_fwd_w, hg_bwd_w, hg_value_w, floor_gap, hg_norm_gain,
    df_query_w, df_key_w, df_value_w, diff_lambda, df_norm_gain, out_hg_w, out_df_w, post_gain,
):
    x = inputs[0]
    tokens, depth = x.shape
    length = tokens * n_sp
    k_rows = hg_query_w.shape[0]
    hr = hg_query_w.shape[1] // HEAD // n_sp
    ha = df_value_w.shape[1] // DFV // n_sp
    columns = 4 * hr * HEAD + ha * (4 * DQK + DFV)
    out_wide = hr * HEAD + ha * DFV
    own_rows = tokens // n_tp
    piece = (columns * k_rows // LANES, LANES)
    low = jnp.bfloat16
    dma = pltpu.SemaphoreType.DMA
    step = n_sp - 1
    turn = n_tp - 1
    out = pl.pallas_call(
        functools.partial(block_kernel, n_sp, n_fs, n_tp, hr, ha),
        out_shape=jax.ShapeDtypeStruct((own_rows, depth), low),
        in_specs=[VMEM_SPEC] * 11
        + [pl.BlockSpec(memory_space=pltpu.SMEM), VMEM_SPEC, ANY_SPEC, ANY_SPEC, VMEM_SPEC],
        out_specs=VMEM_SPEC,
        scratch_shapes=[
            pltpu.VMEM((n_sp,) + piece, low),
            pltpu.VMEM((n_sp, n_fs) + piece, low),
            pltpu.VMEM((n_sp, tokens, depth), low),
            pltpu.VMEM((length, columns), jnp.float32),
            pltpu.VMEM((n_sp, tokens, out_wide), low),
            pltpu.VMEM((n_sp, tokens, out_wide), low),
            pltpu.VMEM((n_tp, own_rows, depth), low),
            pltpu.VMEM((turn, own_rows, depth), low),
            pltpu.VMEM(out_hg_w.shape, low),
            pltpu.VMEM(out_df_w.shape, low),
            dma((2,)),
            dma((step,)), dma((step,)),
            dma((step,)), dma((step,)),
            dma((step, turn)), dma((step, turn)),
            dma((n_sp, n_fs - 1)), dma((n_sp, n_fs - 1)),
            dma((step,)), dma((step,)),
            dma((turn,)), dma((turn,)),
            dma((n_sp, 2)), dma((n_sp, 2)),
        ],
        compiler_params=pltpu.CompilerParams(collective_id=0, has_side_effects=True),
        name="block",
    )(
        x, hg_query_w, hg_fwd_w, hg_bwd_w, hg_value_w, df_query_w, df_key_w, df_value_w,
        norm_gain[None], floor_gap, hg_norm_gain[None], diff_lambda, df_norm_gain[None],
        out_hg_w, out_df_w, post_gain[None],
    )
    return out[None]


def shards(n_sp, n_fs, n_tp, *arrays):
    inputs, hg_query_w, df_value_w = arrays[0], arrays[2], arrays[10]
    heads_hg = hg_query_w.shape[1] // HEAD
    heads_df = df_value_w.shape[1] // DFV
    length = inputs.shape[1] * n_sp
    hr, ha = heads_hg // n_sp, heads_df // n_sp
    whole = heads_hg % n_sp == 0 and heads_df % n_sp == 0 and min(n_sp, n_fs, n_tp) > 1
    aligned = hr * HEAD == LANES and 4 * ha * DQK == LANES and 2 * ha * DFV == LANES
    if whole and aligned and length * STEEPEST < 60.0:
        return headwise_shards(n_sp, n_fs, n_tp, *arrays)
    return spread_shards(*arrays)


def solution(mesh):
    sizes = [mesh.shape[name] for name in ("sp", "fs", "tp")]
    in_specs = (
        P("fs", "sp", None),
        P(),
        P(("sp", "fs"), "tp"),
        P(("sp", "fs"), "tp"),
        P(("sp", "fs"), "tp"),
        P(("sp", "fs"), "tp"),
        P(None, "tp"),
        P(),
        P(("sp", "fs"), "tp"),
        P(("sp", "fs"), "tp"),
        P(("sp", "fs"), "tp"),
        P("tp"),
        P(),
        P("tp", None),
        P("tp", None),
        P(),
    )
    out_specs = P("fs", ("sp", "tp"), None)
    return jax.shard_map(functools.partial(shards, *sizes), mesh=mesh, in_specs=in_specs, out_specs=out_specs, check_vma=False)
```

```python
import functools
import math

import jax
import jax.numpy as jnp
from jax import lax
from jax.experimental import pallas as pl
from jax.experimental.pallas import tpu as pltpu
from jax.sharding import PartitionSpec as P

HEAD = 64
DQK = 32
BLOCK = 64
DFV = 64


epsilon = 1e-06
df_factor = 0.8
highest_precision = lax.Precision.HIGHEST


def rms_scale(values):
    return lax.rsqrt(jnp.mean(values * values, axis=-1, keepdims=True) + epsilon)


def span_scan(queries, taken, values, kept_log):
    head_count, length, key_dim = queries.shape
    blocks = length // BLOCK

    def to_blocks(tensor):
        return tensor.reshape(head_count, blocks, BLOCK, tensor.shape[-1]).transpose(1, 0, 2, 3)

    lower_mask = jnp.tril(jnp.ones((BLOCK, BLOCK), dtype=bool))[:, :, None]

    def advance(state_stack, pieces):
        query_block, key_block, value_block, g_blk = pieces
        cumulative_log = jnp.cumsum(g_blk, axis=1)
        across_blocks = jnp.einsum(
            "bqy,byo->bqo",
            query_block * jnp.exp(cumulative_log),
            state_stack,
            precision=highest_precision,
        )
        spread = cumulative_log[:, :, None, :] - cumulative_log[:, None, :, :]
        decays = jnp.where(lower_mask, jnp.exp(jnp.where(lower_mask, spread, 0.0)), 0.0)
        scores = jnp.einsum(
            "hik,hijk->hij",
            query_block,
            decays * key_block[:, None, :, :],
            precision=highest_precision,
        )
        inside = jnp.einsum("hij,hjv->hiv", scores, value_block, precision=highest_precision)
        final_log_decay = cumulative_log[:, -1:, :]
        carried = jnp.exp(final_log_decay[:, 0, :])[..., None] * state_stack
        fresh_portion = jnp.einsum(
            "moc,moa->mca",
            key_block * jnp.exp(final_log_decay - cumulative_log),
            value_block,
            precision=highest_precision,
        )
        return (carried + fresh_portion, across_blocks + inside)

    start_state = jnp.zeros((head_count, key_dim, values.shape[-1]), jnp.float32)
    final_state, outputs = lax.scan(
        advance,
        start_state,
        (to_blocks(queries), to_blocks(taken), to_blocks(values), to_blocks(kept_log)),
    )
    return (
        outputs.transpose(1, 0, 2, 3).reshape(head_count, length, values.shape[-1]),
        final_state,
    )


def key_width(row_count):
    for candidate in range(min(row_count, 1024), 0, -1):
        if row_count % candidate == 0:
            return candidate
    return 1


def spread_shards(
    inputs,
    norm_gain,
    hg_query_w,
    hg_fwd_w,
    hg_bwd_w,
    hg_value_w,
    floor_gap,
    hg_norm_gain,
    df_query_w,
    df_key_w,
    df_value_w,
    diff_lambda,
    df_norm_gain,
    out_hg_w,
    out_df_w,
    post_gain,
):
    tok_rows = inputs[0]
    length = tok_rows.shape[0]
    rows_float = tok_rows.astype(jnp.float32)
    normed = (rows_float * rms_scale(rows_float) * norm_gain).astype(jnp.bfloat16)
    pieces = (
        lax.all_gather(hg_query_w, ("sp", "fs"), axis=0, tiled=True),
        lax.all_gather(hg_fwd_w, ("sp", "fs"), axis=0, tiled=True),
        lax.all_gather(hg_bwd_w, ("sp", "fs"), axis=0, tiled=True),
        lax.all_gather(hg_value_w, ("sp", "fs"), axis=0, tiled=True),
        lax.all_gather(df_query_w, ("sp", "fs"), axis=0, tiled=True),
        lax.all_gather(df_key_w, ("sp", "fs"), axis=0, tiled=True),
        lax.all_gather(df_value_w, ("sp", "fs"), axis=0, tiled=True),
    )
    summed = tuple((jnp.dot(normed, piece, preferred_element_type=jnp.float32) for piece in pieces))
    hg_query, hg_fwd, hg_bwd, hg_value, df_query, df_key, df_value = [
        member.astype(jnp.bfloat16) for member in summed
    ]
    heads_hg = hg_query.shape[1] // HEAD

    def split_heads(tensor):
        return tensor.astype(jnp.float32).reshape(length, heads_hg, HEAD).transpose(1, 0, 2)

    queries = jax.nn.silu(split_heads(hg_query))
    values = split_heads(hg_value)

    def summarize(raw_gate, gap_row, flipped):
        taken = gap_row.reshape(heads_hg, 1, HEAD) * jax.nn.sigmoid(-split_heads(raw_gate))
        series = (queries, taken, values, jnp.log1p(-taken))
        if flipped:
            series = tuple((jnp.flip(tensor, axis=1) for tensor in series))
        local_out, final_state = span_scan(*series)
        cumulative_log = jnp.cumsum(series[3], axis=1)
        return (
            local_out,
            final_state,
            jnp.exp(cumulative_log[:, -1, :]),
            series[0] * jnp.exp(cumulative_log),
        )

    forward_output, fwd_state, fwd_decay, forward_reader = summarize(hg_fwd, floor_gap[0], False)
    backward_output, bwd_state, bwd_decay, backward_reader = summarize(hg_bwd, floor_gap[1], True)
    all_decay, all_state = (
        lax.all_gather(
            jnp.stack([fwd_decay, bwd_decay])[None].astype(jnp.bfloat16), "sp", axis=0, tiled=True
        ).astype(jnp.float32),
        lax.all_gather(
            jnp.stack([fwd_state, bwd_state])[None].astype(jnp.bfloat16), "sp", axis=0, tiled=True
        ).astype(jnp.float32),
    )
    position = lax.axis_index("sp")
    members = all_decay.shape[0]

    def forward_step(member, running):
        joined = all_decay[member, 0][..., None] * running + all_state[member, 0]
        return jnp.where(member < position, joined, running)

    def backward_step(offset, running):
        member = members - 1 - offset
        joined = all_decay[member, 1][..., None] * running + all_state[member, 1]
        return jnp.where(member > position, joined, running)

    forward_carry = lax.fori_loop(0, members, forward_step, jnp.zeros_like(fwd_state))
    backward_carry = lax.fori_loop(0, members, backward_step, jnp.zeros_like(bwd_state))
    forward_sum = forward_output + jnp.einsum(
        "bqy,byo->bqo", forward_reader, forward_carry, precision=highest_precision
    )
    bwd_total = jnp.flip(
        backward_output
        + jnp.einsum("bqy,byo->bqo", backward_reader, backward_carry, precision=highest_precision),
        axis=1,
    )
    recurrent = forward_sum + bwd_total
    hg_out = (
        (recurrent * rms_scale(recurrent) * hg_norm_gain)
        .transpose(1, 0, 2)
        .reshape(length, heads_hg * HEAD)
        .astype(jnp.bfloat16)
    )
    heads_df = df_value.shape[1] // DFV
    df_queries = df_query.reshape(length, heads_df, 2, DQK)
    score_scale = DQK ** (-0.5)
    start_carry = (
        jnp.full((heads_df, 2, length), -1e30, jnp.float32),
        jnp.zeros((heads_df, 2, length), jnp.float32),
        jnp.zeros((heads_df, 2, length, DFV), jnp.float32),
    )
    carry = start_carry
    key_rows = lax.all_gather(df_key, "sp", axis=0, tiled=True)
    value_rows = lax.all_gather(df_value, "sp", axis=0, tiled=True)
    row_count = key_rows.shape[0]
    block_rows = key_width(row_count)
    key_blocks = key_rows.reshape(row_count // block_rows, block_rows, heads_df, 2, DQK)
    value_blocks = value_rows.reshape(row_count // block_rows, block_rows, heads_df, DFV)

    def key_step(running, block_pair):
        tops, totals, accums = running
        key_blk, value_blk = block_pair
        scores = (
            jnp.einsum("qhmd,khmd->hmqk", df_queries, key_blk, preferred_element_type=jnp.float32)
            * score_scale
        )
        new_tops = jnp.maximum(tops, jnp.max(scores, axis=-1))
        factor = jnp.exp(tops - new_tops)
        weights_blk = jnp.exp(scores - new_tops[..., None])
        totals = totals * factor + jnp.sum(weights_blk, axis=-1)
        accums = accums * factor[..., None] + jnp.einsum(
            "hmqk,khd->hmqd",
            weights_blk.astype(jnp.bfloat16),
            value_blk,
            preferred_element_type=jnp.float32,
        )
        return ((new_tops, totals, accums), None)

    carry, unused = lax.scan(key_step, carry, (key_blocks, value_blocks))
    tops, totals, accums = carry
    maps = accums / totals[..., None]
    weighted = maps[:, 0] - diff_lambda[:, None, None] * maps[:, 1]
    df_out = (
        (weighted * rms_scale(weighted) * df_norm_gain * df_factor)
        .transpose(1, 0, 2)
        .reshape(length, heads_df * DFV)
        .astype(jnp.bfloat16)
    )
    mixture = lax.psum_scatter(
        (
            jnp.dot(hg_out, out_hg_w, preferred_element_type=jnp.float32)
            + jnp.dot(df_out, out_df_w, preferred_element_type=jnp.float32)
        ).astype(jnp.bfloat16),
        "tp",
        scatter_dimension=0,
        tiled=True,
    ).astype(jnp.float32)
    return (mixture * rms_scale(mixture) * post_gain).astype(jnp.bfloat16)[None]


MESH = pl.DeviceIdType.MESH
VMEM_SPEC = pl.BlockSpec(memory_space=pltpu.VMEM)
ANY_SPEC = pl.BlockSpec(memory_space=pl.ANY)
STEEPEST = -math.log1p(-0.1)


LANES = 128


def remote(src, dst, send, recv, peer):
    return pltpu.make_async_remote_copy(
        src_ref=src, dst_ref=dst, send_sem=send, recv_sem=recv, device_id=peer, device_id_type=MESH
    )


def recurrence(proj_ref, gap, hgain, hr, store):
    length = proj_ref.shape[0]
    wide = hr * HEAD
    hq = proj_ref[:, 0:wide].astype(jnp.bfloat16).astype(jnp.float32)
    hf = proj_ref[:, wide : 2 * wide].astype(jnp.bfloat16).astype(jnp.float32)
    hb = proj_ref[:, 2 * wide : 3 * wide].astype(jnp.bfloat16).astype(jnp.float32)
    hv = proj_ref[:, 3 * wide : 4 * wide].astype(jnp.bfloat16)
    queries = hq * jax.nn.sigmoid(hq)
    taken_f = gap[0:1, :] * jax.nn.sigmoid(-hf)
    taken_b = gap[1:2, :] * jax.nn.sigmoid(-hb)
    kept_b = jnp.log1p(-taken_b)
    kept = jnp.concatenate([jnp.log1p(-taken_f), kept_b], axis=1)
    row = lax.broadcasted_iota(jnp.int32, (length, length), 0)
    col = lax.broadcasted_iota(jnp.int32, (length, length), 1)
    lower = row >= col
    upper = row <= col
    ones = jnp.where(lower, 1.0, 0.0).astype(jnp.bfloat16)
    cumulative = jnp.zeros_like(kept)
    rest = kept
    for _ in range(3):
        part = rest.astype(jnp.bfloat16)
        rest = rest - part.astype(jnp.float32)
        cumulative = cumulative + jnp.dot(ones, part, preferred_element_type=jnp.float32)
    before = cumulative[:, wide:] - kept_b
    after = cumulative[:, :wide]
    after = after - 0.5 * after[length - 1 : length, :]
    before = before - 0.5 * before[length - 1 : length, :]
    qf = (queries * jnp.exp(after)).astype(jnp.bfloat16)
    kf = (taken_f * jnp.exp(-after)).astype(jnp.bfloat16)
    qb = (queries * jnp.exp(-before)).astype(jnp.bfloat16)
    kb = (taken_b * jnp.exp(before)).astype(jnp.bfloat16)
    across = (((1,), (1,)), ((), ()))
    for h in range(hr):
        span = slice(h * HEAD, (h + 1) * HEAD)
        fwd = lax.dot_general(qf[:, span], kf[:, span], across, preferred_element_type=jnp.float32)
        bwd = lax.dot_general(qb[:, span], kb[:, span], across, preferred_element_type=jnp.float32)
        scores = jnp.where(lower, fwd, 0.0) + jnp.where(upper, bwd, 0.0)
        out = jnp.dot(scores.astype(jnp.bfloat16), hv[:, span], preferred_element_type=jnp.float32)
        scale = lax.rsqrt(jnp.mean(out * out, axis=-1, keepdims=True) + epsilon)
        store(span.start, (out * scale * hgain).astype(jnp.bfloat16))


def attention(proj_ref, first_lam, lam_ref, dgain, q_at, ha, out_at, store):
    across = (((1,), (1,)), ((), ()))
    k_at = q_at + ha * 2 * DQK
    v_at = k_at + ha * 2 * DQK
    for h in range(ha):
        value = proj_ref[:, v_at + h * DFV : v_at + (h + 1) * DFV].astype(jnp.bfloat16)
        maps = []
        for m in range(2):
            offset = (h * 2 + m) * DQK
            query = proj_ref[:, q_at + offset : q_at + offset + DQK].astype(jnp.bfloat16)
            key = proj_ref[:, k_at + offset : k_at + offset + DQK].astype(jnp.bfloat16)
            scores = lax.dot_general(
                query, key, across, preferred_element_type=jnp.float32
            ) * (DQK ** (-0.5))
            shifted = jnp.exp(scores - jnp.max(scores, axis=-1, keepdims=True))
            total = jnp.sum(shifted, axis=-1, keepdims=True)
            accum = jnp.dot(shifted.astype(jnp.bfloat16), value, preferred_element_type=jnp.float32)
            maps.append(accum / total)
        weighted = maps[0] - lam_ref[first_lam + h] * maps[1]
        scale = lax.rsqrt(jnp.mean(weighted * weighted, axis=-1, keepdims=True) + epsilon)
        store(out_at + h * DFV, (weighted * scale * dgain * df_factor).astype(jnp.bfloat16))


def block_kernel(
    n_sp, n_fs, n_tp, hr, ha,
    x_ref, w0, w1, w2, w3, w4, w5, w6, gain_ref, gap_ref, hgain_ref, lam_ref, dgain_ref,
    wh_hbm, wd_hbm, post_ref, out_ref,
    wp, wg, w_all, xg, proj, ob, og, pbuf, rbuf, wh, wd,
    local, s1, r1, sx, rx, sy, ry, s2, r2, s3, r3, s4, r4, s5, r5,
):
    sp, fs, tp = lax.axis_index("sp"), lax.axis_index("fs"), lax.axis_index("tp")
    if n_sp == 4:
        near, far = lax.rem(sp, 2), sp // 2
        sp_peers = [far * 2 + 1 - near, (1 - far) * 2 + near, n_sp - 1 - sp]
        sp_froms = sp_peers
    else:
        sp_peers = [lax.rem(sp + d, n_sp) for d in range(1, n_sp)]
        sp_froms = [lax.rem(sp + n_sp - d, n_sp) for d in range(1, n_sp)]
    tp_peers = [lax.rem(tp + d, n_tp) for d in range(1, n_tp)]
    tp_froms = [lax.rem(tp + n_tp - d, n_tp) for d in range(1, n_tp)]
    paired = n_fs == 4
    if paired:
        low, high = lax.rem(fs, 2), fs // 2
        fs_peers = [high * 2 + 1 - low, (1 - high) * 2 + low]
        fs_froms = fs_peers
    else:
        fs_peers = [lax.rem(fs + e, n_fs) for e in range(1, n_fs)]
        fs_froms = [lax.rem(fs + n_fs - e, n_fs) for e in range(1, n_fs)]
    barrier = pltpu.get_barrier_semaphore()
    peers = (
        [{"sp": p} for p in sp_peers] + [{"fs": p} for p in fs_peers] + [{"tp": p} for p in tp_peers]
    )
    for peer in peers:
        pl.semaphore_signal(barrier, inc=1, device_id=peer, device_id_type=MESH)
    load_wh = pltpu.make_async_copy(wh_hbm, wh, local.at[0])
    load_wd = pltpu.make_async_copy(wd_hbm, wd, local.at[1])
    tokens, depth = x_ref.shape
    k_rows = w0.shape[0]
    wide = hr * HEAD
    thin = ha * DFV
    half = k_rows // 2
    for s in range(n_sp):
        for b, w in enumerate((w0, w1, w2, w3)):
            wp[s, b * k_rows : (b + 1) * k_rows, :] = w[:, s * wide : (s + 1) * wide]
        cut = slice(s * thin, (s + 1) * thin)
        wp[s, 4 * k_rows : 5 * k_rows, :] = jnp.concatenate([w4[:, cut], w5[:, cut]], axis=1)
        wp[s, 5 * k_rows :, :] = jnp.concatenate([w6[:half, cut], w6[half:, cut]], axis=1)
    pl.semaphore_wait(barrier, len(peers))

    started = []

    def send(*args):
        copy = remote(*args)
        copy.start()
        started.append(copy)
        return copy

    along = [
        send(wp.at[peer], wg.at[sp, fs], s1.at[d], r1.at[d], {"sp": peer})
        for d, peer in enumerate(sp_peers)
    ]
    across_fs = [
        [
            send(wp.at[sp], wg.at[sp, fs], s2.at[0, e], r2.at[0, e], {"fs": peer})
            for e, peer in enumerate(fs_peers)
        ]
    ]
    share = tokens // n_tp
    mine = pl.ds(pl.multiple_of(tp * share, share), share)

    has = (sp + 1 < n_sp, sp > 0)
    toward = (lax.rem(sp + 1, n_sp), lax.rem(sp + n_sp - 1, n_sp))

    def holds(way, hops):
        return sp >= hops if way == 0 else sp + hops < n_sp

    def origin(way, hops):
        return lax.rem(sp + n_sp - hops, n_sp) if way == 0 else lax.rem(sp + hops, n_sp)

    def hop(way, hops):
        source = origin(way, hops)
        place = xg.at[source, mine, :]
        src = x_ref.at[mine, :] if hops == 0 else place
        return remote(src, place, sx.at[way, hops], rx.at[way, hops], {"sp": toward[way]})

    def hand(way, hops, e):
        part = xg.at[origin(way, hops + 1), mine, :]
        return remote(part, part, sy.at[way, hops, e], ry.at[way, hops, e], {"tp": tp_peers[e]})

    def push(hops):
        for way in range(2):
            @pl.when(holds(way, hops) & has[way])
            def _():
                hop(way, hops).start()

    def take(hops):
        for way in range(2):
            @pl.when(holds(way, hops + 1))
            def _():
                hop(way, hops).wait_recv()
                if hops + 1 < n_sp - 1:
                    @pl.when(has[way])
                    def _():
                        hop(way, hops + 1).start()
                for e in range(n_tp - 1):
                    hand(way, hops, e).start()

    def finish(hops):
        for way in range(2):
            @pl.when(holds(way, hops + 1))
            def _():
                for e in range(n_tp - 1):
                    hand(way, hops, e).wait()
                if hops + 1 < n_sp - 1:
                    @pl.when(has[way])
                    def _():
                        hop(way, hops + 1).wait_send()
                source = origin(way, hops + 1)
                normalize(source, xg[source])

    push(0)
    load_wh.start()
    load_wd.start()

    piece_rows = wp.shape[1]
    cuts = (slice(0, piece_rows // 2), slice(piece_rows // 2, piece_rows))
    relays = []

    def spread(k):
        along[k - 1].wait_recv()
        piece = wg.at[sp_froms[k - 1], fs]
        across_fs.append(
            [
                send(piece, piece, s2.at[k, e], r2.at[k, e], {"fs": peer})
                for e, peer in enumerate(fs_peers)
            ]
        )

    def relay(k):
        source = sp if k == 0 else sp_froms[k - 1]
        for e, copy in enumerate(across_fs[k]):
            copy.wait_recv()
            if paired:
                piece = wg.at[source, fs_peers[e], cuts[e], :]
                relays.append(
                    (k, send(piece, piece, s5.at[k, e], r5.at[k, e], {"fs": fs_peers[1 - e]}))
                )

    def normalize(s, rows):
        x = rows.astype(jnp.float32)
        scale = lax.rsqrt(jnp.mean(x * x, axis=-1, keepdims=True) + epsilon)
        xg[s] = (x * scale * gain_ref[...]).astype(jnp.bfloat16)

    def assemble(k):
        source = sp if k == 0 else sp_froms[k - 1]
        for at, copy in relays:
            if at == k:
                copy.wait_recv()
        for f in range(n_fs):
            first = source * (n_fs * k_rows) + f * k_rows
            for b in range(5):
                w_all[pl.ds(pl.multiple_of(first, half), k_rows), b * LANES : (b + 1) * LANES] = wg[
                    source, f, b * k_rows : (b + 1) * k_rows, :
                ]
            tail = wg[source, f, 5 * k_rows :, :]
            w_all[pl.ds(pl.multiple_of(first, half), half), 5 * LANES :] = tail[:, :thin]
            w_all[pl.ds(pl.multiple_of(first + half, half), half), 5 * LANES :] = tail[:, thin:]

    wg[sp, fs] = wp[sp]
    normalize(sp, x_ref[...])
    for k in range(1, n_sp):
        spread(k)
        relay(k - 1)
    take(0)
    assemble(0)
    relay(n_sp - 1)
    for hops in range(1, n_sp - 1):
        assemble(hops)
        take(hops)
    finish(0)
    assemble(n_sp - 1)
    for hops in range(1, n_sp - 1):
        finish(hops)
    proj[...] = jnp.dot(
        xg[...].reshape(n_sp * tokens, depth), w_all[...], preferred_element_type=jnp.float32
    )

    def store(at, block):
        width = block.shape[1]
        for s in range(n_sp):
            ob[s, :, at : at + width] = block[s * tokens : (s + 1) * tokens]

    gap = gap_ref[:, pl.ds(pl.multiple_of(sp * wide, LANES), wide)]
    recurrence(proj, gap, hgain_ref[...], hr, store)
    attention(proj, sp * ha, lam_ref, dgain_ref[...], 4 * wide, ha, wide, store)

    heads = [
        send(ob.at[peer], og.at[sp], s3.at[d], r3.at[d], {"sp": peer})
        for d, peer in enumerate(sp_peers)
    ]
    og[sp] = ob[sp]
    load_wh.wait()
    load_wd.wait()
    for copy in heads:
        copy.wait_recv()
    hg = jnp.concatenate([og[s, :, :wide] for s in range(n_sp)], axis=1)
    df = jnp.concatenate([og[s, :, wide:] for s in range(n_sp)], axis=1)
    partial = jnp.dot(hg, wh[...], preferred_element_type=jnp.float32) + jnp.dot(
        df, wd[...], preferred_element_type=jnp.float32
    )
    pbuf[...] = partial.astype(jnp.bfloat16).reshape(pbuf.shape)
    sums = [
        send(pbuf.at[peer], rbuf.at[d], s4.at[d], r4.at[d], {"tp": peer})
        for d, peer in enumerate(tp_peers)
    ]
    mixture = pbuf[tp].astype(jnp.float32)
    for d, copy in enumerate(sums):
        copy.wait_recv()
        mixture = mixture + rbuf[d].astype(jnp.float32)
    scale = lax.rsqrt(jnp.mean(mixture * mixture, axis=-1, keepdims=True) + epsilon)
    out_ref[...] = (mixture * scale * post_ref[...]).astype(jnp.bfloat16)
    for copy in started:
        copy.wait_send()
    for way in range(2):
        @pl.when(has[way])
        def _():
            hop(way, 0).wait_send()


def headwise_shards(
    n_sp, n_fs, n_tp,
    inputs, norm_gain, hg_query_w, hg_fwd_w, hg_bwd_w, hg_value_w, floor_gap, hg_norm_gain,
    df_query_w, df_key_w, df_value_w, diff_lambda, df_norm_gain, out_hg_w, out_df_w, post_gain,
):
    x = inputs[0]
    tokens, depth = x.shape
    length = tokens * n_sp
    k_rows = hg_query_w.shape[0]
    hr = hg_query_w.shape[1] // HEAD // n_sp
    ha = df_value_w.shape[1] // DFV // n_sp
    columns = 4 * hr * HEAD + ha * (4 * DQK + DFV)
    out_wide = hr * HEAD + ha * DFV
    own_rows = tokens // n_tp
    piece = (columns * k_rows // LANES, LANES)
    low = jnp.bfloat16
    dma = pltpu.SemaphoreType.DMA
    step = n_sp - 1
    turn = n_tp - 1
    out = pl.pallas_call(
        functools.partial(block_kernel, n_sp, n_fs, n_tp, hr, ha),
        out_shape=jax.ShapeDtypeStruct((own_rows, depth), low),
        in_specs=[VMEM_SPEC] * 11
        + [pl.BlockSpec(memory_space=pltpu.SMEM), VMEM_SPEC, ANY_SPEC, ANY_SPEC, VMEM_SPEC],
        out_specs=VMEM_SPEC,
        scratch_shapes=[
            pltpu.VMEM((n_sp,) + piece, low),
            pltpu.VMEM((n_sp, n_fs) + piece, low),
            pltpu.VMEM((n_sp * n_fs * k_rows, columns), low),
            pltpu.VMEM((n_sp, tokens, depth), low),
            pltpu.VMEM((length, columns), jnp.float32),
            pltpu.VMEM((n_sp, tokens, out_wide), low),
            pltpu.VMEM((n_sp, tokens, out_wide), low),
            pltpu.VMEM((n_tp, own_rows, depth), low),
            pltpu.VMEM((turn, own_rows, depth), low),
            pltpu.VMEM(out_hg_w.shape, low),
            pltpu.VMEM(out_df_w.shape, low),
            dma((2,)),
            dma((step,)), dma((step,)),
            dma((2, step)), dma((2, step)),
            dma((2, step, turn)), dma((2, step, turn)),
            dma((n_sp, n_fs - 1)), dma((n_sp, n_fs - 1)),
            dma((step,)), dma((step,)),
            dma((turn,)), dma((turn,)),
            dma((n_sp, 2)), dma((n_sp, 2)),
        ],
        compiler_params=pltpu.CompilerParams(collective_id=0, has_side_effects=True),
        name="block",
    )(
        x, hg_query_w, hg_fwd_w, hg_bwd_w, hg_value_w, df_query_w, df_key_w, df_value_w,
        norm_gain[None], floor_gap, hg_norm_gain[None], diff_lambda, df_norm_gain[None],
        out_hg_w, out_df_w, post_gain[None],
    )
    return out[None]


def shards(n_sp, n_fs, n_tp, *arrays):
    inputs, hg_query_w, df_value_w = arrays[0], arrays[2], arrays[10]
    heads_hg = hg_query_w.shape[1] // HEAD
    heads_df = df_value_w.shape[1] // DFV
    length = inputs.shape[1] * n_sp
    hr, ha = heads_hg // n_sp, heads_df // n_sp
    whole = heads_hg % n_sp == 0 and heads_df % n_sp == 0 and min(n_sp, n_fs, n_tp) > 1
    aligned = hr * HEAD == LANES and 4 * ha * DQK == LANES and 2 * ha * DFV == LANES
    if whole and aligned and length * STEEPEST < 60.0:
        return headwise_shards(n_sp, n_fs, n_tp, *arrays)
    return spread_shards(*arrays)


def solution(mesh):
    sizes = [mesh.shape[name] for name in ("sp", "fs", "tp")]
    in_specs = (
        P("fs", "sp", None),
        P(),
        P(("sp", "fs"), "tp"),
        P(("sp", "fs"), "tp"),
        P(("sp", "fs"), "tp"),
        P(("sp", "fs"), "tp"),
        P(None, "tp"),
        P(),
        P(("sp", "fs"), "tp"),
        P(("sp", "fs"), "tp"),
        P(("sp", "fs"), "tp"),
        P("tp"),
        P(),
        P("tp", None),
        P("tp", None),
        P(),
    )
    out_specs = P("fs", ("sp", "tp"), None)
    return jax.shard_map(functools.partial(shards, *sizes), mesh=mesh, in_specs=in_specs, out_specs=out_specs, check_vma=False)
```
